768 devices in a mesh: ep: 48 (over z, x), tp: 16 (over y, core).
Axes of the slice: x: 4, y: 8, z: 12, core: 2. Of those that a mesh axis runs over, the one named last changes fastest.
Arguments:
- tokens: bfloat16 [122880, 2048], P(('ep', 'tp')), may hold values from -6 to 6
- expert_ids: int32 [122880, 2], P(('ep', 'tp')), may hold values from 0 to 47, all different within a row; in each aligned block of 160 rows (0 to 159, 160 to 319, ...) at most 10 rows name the same one
- group_weight: float32 [122880], P(('ep', 'tp')), may hold values from 0.3 to 1
- expert_share: float32 [122880, 2], P(('ep', 'tp')), may hold values from 0.05 to 1
- gate_w: bfloat16 [48, 512, 2048], P('ep', 'tp'), may hold values from -0.125 to 0.125
- up_w: bfloat16 [48, 512, 2048], P('ep', 'tp'), may hold values from -0.125 to 0.125
- down_w: bfloat16 [48, 512, 2048], P('ep', 'tp'), may hold values from -0.25 to 0.25
- out_gain: float32 [2048], replicated, may hold values from 0.1 to 1.9
- out_shift: float32 [2048], replicated, may hold values from -3 to 3
Outputs:
- layer_out: bfloat16 [122880, 2048], P(('ep', 'tp'))
The draws below stay inside these ranges and needn't reach their ends.
Inputs may be any that keep to these rules, and one draw needn't show every extreme that they name: `expert_ids`: the 2 ids of a token differ. Among the rows of one device no id is named more than 10 times, and in some device's rows some id is named exactly 10 times.
All inputs are finite; a program needn't handle non-finite values.
Results may differ from the reference program's by a relative error of at most 0.0021.
Values may be sent and summed in bfloat16 or wider, within the bound.
No kernel may reach another device: no remote copies, remote signals or barrier semaphores. Data moves between devices by JAX's collectives and lax.ppermute only.
A program may use at most 32 MiB of HBM per device.

```python
import math
import jax
import jax.numpy as jnp
import numpy as np
from jax import lax

D = 2048
FF = 512
TOP = 2
TOK_DEV = 160
EXPERTS = 48
CAP = 10
TOKENS = 122880
N_EP = 48
N_TP = 16


def block_scale(key, extent, cuts, least, top_value):
    def one(dim, blocks):
        draws = jax.random.uniform(jax.random.fold_in(jax.random.fold_in(key, 6), dim), (blocks,), jnp.float32, least / len(cuts), top_value / len(cuts))
        return jnp.repeat(jnp.exp(draws), extent[dim] // blocks).reshape((-1,) + (1,) * (len(extent) - dim - 1))

    loudness = one(*cuts[0])
    for cut in cuts[1:]:
        loudness = loudness * one(*cut)
    return loudness


def assign_block(key, own, number, rows, amount, top, reach, skew):
    sequence = jax.random.permutation(key, amount)
    crowded, common = shares(amount, rows * top, reach, skew, True), shares(amount, rows * top, reach, skew, False)
    places = jnp.arange(amount)

    def named(sizes, offset_by):
        used = int((sizes > 0).sum())
        fixed = max(1, used // 4)
        shifted = fixed + (places - fixed + offset_by * (used - fixed)) % max(1, amount - fixed)
        return jnp.zeros((amount,), jnp.int32).at[sequence[jnp.where(places < fixed, places, shifted)]].set(jnp.asarray(sizes, jnp.int32))

    sizes = jnp.where(number % 4 == 0, named(crowded, number // 4), named(common, number - number // 4 - 1))
    mixed = jax.random.permutation(jax.random.fold_in(own, 3), amount)
    source_of, receiver = mixed[0:amount // 2 * 2:2], mixed[1:amount // 2 * 2:2]
    slack = jnp.minimum(sizes[source_of] - 1, reach - sizes[receiver]) // 2
    slack = jnp.where((source_of == sequence[0]) | (receiver == sequence[0]) | (sizes[receiver] == 0), 0, jnp.maximum(slack, 0))
    shifted = jax.random.randint(jax.random.fold_in(own, 4), (amount // 2,), 0, 1 << 20) % (slack + 1)
    sizes = sizes.at[source_of].add(-shifted).at[receiver].add(shifted)
    items = jnp.searchsorted(jnp.cumsum(sizes), jnp.arange(rows * top), side="right").astype(jnp.int32)
    table = items.reshape(top, rows).T
    table = table[jax.random.permutation(jax.random.fold_in(own, 1), rows)]
    offset_by = jax.random.randint(jax.random.fold_in(own, 2), (rows, 1), 0, top)
    return jnp.take_along_axis(table, (jnp.arange(top)[None, :] + offset_by) % top, axis=1)


def shares(amount, total, reach, lean, full):
    weights = [(1 << 20) // math.isqrt(rank ** lean) + 1 for rank in range(1, amount + 1)]
    largest = reach if full else min(reach, max(-(-total // amount), total * weights[0] // sum(weights)))
    least = 1 if total - largest >= amount - 1 else 0
    given, rest = [largest] + [least] * (amount - 1), total - largest - least * (amount - 1)
    while rest > 0:
        movable = [i for i in range(1, amount) if given[i] < largest] or [i for i in range(1, amount) if given[i] < reach]
        pool, budget = sum([weights[i] for i in movable]), rest
        for i in movable:
            more = min(reach - given[i], max(1, budget * weights[i] // pool), rest)
            given[i] = given[i] + more
            rest = rest - more
    return np.array(given)


def centred(stream_key, shape, spread, limit, pieces=(), held_as=jnp.bfloat16):
    result = jax.random.normal(stream_key, shape, jnp.float32) * spread
    if len(pieces) > 0:
        result = block_scale(stream_key, shape, pieces, -0.22, 0.18) * result
    return jnp.clip(result, min=-limit, max=limit).astype(held_as)


def setup_inputs(seed: int = 0) -> dict:
    streams_of = jax.random.split(jax.random.key(seed), 10)
    tokens = centred(streams_of[0], (TOKENS, D), 1.0, 6.0, ((0, 768),))
    expert_ids_keys = jax.random.split(jax.random.fold_in(streams_of[1], 1), TOKENS // TOK_DEV)
    expert_ids_turns = jax.random.permutation(jax.random.fold_in(streams_of[1], 3), TOKENS // TOK_DEV)
    expert_ids = jax.vmap(lambda own, number: assign_block(jax.random.fold_in(streams_of[1], 2), own, number, TOK_DEV, EXPERTS, TOP, CAP, 2))(expert_ids_keys, expert_ids_turns).reshape((TOKENS, TOP))
    group_weight = jnp.clip(0.3 + 0.7 * jax.random.uniform(streams_of[2], (TOKENS,), jnp.float32) ** block_scale(streams_of[2], (TOKENS,), ((0, 768),), -0.2, 0.2), 0.3, 1.0)
    expert_share = jnp.clip(jnp.exp(math.log(1.0) - 2.9957323 * jax.random.uniform(streams_of[3], (TOKENS, TOP), jnp.float32) ** block_scale(streams_of[3], (TOKENS, TOP), ((0, 768),), -0.2, 0.2)), 0.05, 1.0)
    gate_w = centred(streams_of[4], (EXPERTS, FF, D), D ** -0.5, 0.125, ((0, 48), (1, 16)))
    up_w = centred(streams_of[5], (EXPERTS, FF, D), D ** -0.5, 0.125, ((0, 48), (1, 16)))
    down_w = centred(streams_of[6], (EXPERTS, FF, D), FF ** -0.5, 0.25, ((0, 48), (1, 16)))
    out_gain = jnp.clip(1.0 + 0.18 * jax.random.normal(streams_of[7], (D,), jnp.float32), 0.1, 1.9)
    out_shift = centred(streams_of[8], (D,), 0.5, 3.0, (), jnp.float32)
    return {"tokens": tokens, "expert_ids": expert_ids, "group_weight": group_weight, "expert_share": expert_share, "gate_w": gate_w, "up_w": up_w, "down_w": down_w, "out_gain": out_gain, "out_shift": out_shift}


residual_scale = 2.0 ** 0.5
norm_eps = 1e-05

def layer_norm(values, gain, shift):
    center = values - lax.optimization_barrier(jnp.mean(values, axis=-1, keepdims=True))
    variance = lax.optimization_barrier(jnp.mean(center * center, axis=-1, keepdims=True))
    return (center * lax.rsqrt(variance + norm_eps) * gain + shift).astype(jnp.bfloat16)

def reference(tokens, expert_ids, group_weight, expert_share, gate_w, up_w, down_w, out_gain, out_shift):
    tok_count = tokens.shape[0]
    model_width = tokens.shape[1]
    row_limit = N_EP * N_TP * CAP
    share_norm = expert_share / lax.optimization_barrier(jnp.sum(expert_share, axis=1, keepdims=True))
    route_weight = group_weight[:, None] * share_norm
    padded = jnp.concatenate([tokens, jnp.zeros((1, model_width), tokens.dtype)], axis=0)

    def one_expert(carry, expert_num):
        is_hit = expert_ids == expert_num
        weight_col = lax.optimization_barrier(jnp.sum(jnp.where(is_hit, route_weight, 0.0), axis=1))
        token_mask = jnp.any(is_hit, axis=1)
        row_index = jnp.nonzero(token_mask, size=row_limit, fill_value=tok_count)[0].astype(jnp.int32)
        row_data = padded[row_index]
        gate_act = jnp.dot(row_data, gate_w[expert_num].T, preferred_element_type=jnp.float32)
        up_act = jnp.dot(row_data, up_w[expert_num].T, preferred_element_type=jnp.float32)
        hidden = (jax.nn.silu(gate_act) * up_act).astype(jnp.bfloat16)
        expert_out = jnp.dot(hidden, down_w[expert_num], preferred_element_type=jnp.float32).astype(jnp.bfloat16)
        padded_weight = jnp.concatenate([weight_col, jnp.zeros((1,), weight_col.dtype)])[row_index]
        carry = carry.at[row_index].add(padded_weight[:, None] * expert_out.astype(jnp.float32))
        return (carry, None)
    start_total = jnp.zeros((tok_count + 1, model_width), jnp.float32)
    mixture, _ = lax.scan(one_expert, start_total, jnp.arange(EXPERTS, dtype=jnp.int32))
    residual = residual_scale * tokens.astype(jnp.float32) + mixture[:tok_count]
    return layer_norm(residual, out_gain, out_shift)
```

```python
import functools

import jax
import jax.numpy as jnp
from jax import lax
from jax.experimental import pallas as pl
from jax.experimental.pallas import tpu as pltpu
from jax.sharding import PartitionSpec as P

TOP = 2
residual_scale = 2.0**0.5
norm_eps = 1e-05
BF16 = jnp.bfloat16
F32 = jnp.float32
HEAD = 8
REST = 2
QUARTERS = 4


def dot(a, b):
    return jnp.dot(a, b, preferred_element_type=F32)


def dot_nt(a, b):
    return lax.dot_general(a, b, (((1,), (1,)), ((), ())), preferred_element_type=F32)


def iota(shape, dim):
    return lax.broadcasted_iota(jnp.int32, shape, dim)


def flag(condition):
    return jnp.where(condition, 1.0, 0.0).astype(BF16)


def pack_kernel(tok_ref, ids_ref, out_ref):
    experts, _, width = out_ref.shape
    count = tok_ref.shape[0]
    expert = iota((experts, count), 0)
    named = (ids_ref[0:1, :] == expert) | (ids_ref[1:2, :] == expert)
    hit = jnp.where(named, 1.0, 0.0)
    before = flag(iota((count, count), 0) < iota((count, count), 1))
    place = hit * (dot(hit.astype(BF16), before) + 1.0)
    slots = experts * HEAD
    spread = flag(iota((slots, experts), 0) // HEAD == iota((slots, experts), 1))
    place = dot(spread, place.astype(BF16))
    row = iota((slots, count), 0)
    in_block = row % HEAD
    head = flag(place == (in_block + 1).astype(F32))
    second = place == (HEAD + 1 + row % REST).astype(F32)
    rest = jnp.zeros((slots, width), F32)
    for q in range(QUARTERS):
        part = tok_ref[:, q * width : (q + 1) * width]
        out_ref[:, q * HEAD : (q + 1) * HEAD, :] = (
            dot(head, part).astype(BF16).reshape(experts, HEAD, width)
        )
        rest += dot(flag(second & (in_block // REST == q)), part)
    out_ref[:, QUARTERS * HEAD :, :] = rest.astype(BF16).reshape(experts, HEAD, width)


def ffn_kernel(gate_steps, recv_ref, gate_ref, up_ref, down_ref, out_ref, rows_ref, hidden_ref, rest_ref):
    step = pl.program_id(0)
    sources, _, width = recv_ref.shape
    heads, rests = sources * HEAD, sources * REST

    def pick(q):
        a = iota((rests, heads), 0)
        return flag(iota((rests, heads), 1) == (a // REST) * HEAD + q * REST + a % REST)

    def spread(q):
        a = iota((heads, rests), 1)
        return flag(iota((heads, rests), 0) == (a // REST) * HEAD + q * REST + a % REST)

    @pl.when(step == 0)
    def _():
        rest = recv_ref[:, QUARTERS * HEAD :, :].reshape(heads, width)
        for q in range(QUARTERS):
            cols = slice(q * width, (q + 1) * width)
            rows_ref[0:heads, cols] = recv_ref[:, q * HEAD : (q + 1) * HEAD, :].reshape(heads, width)
            rows_ref[heads:, cols] = dot(pick(q), rest).astype(BF16)

    for i in range(gate_steps):

        @pl.when(step == i)
        def _():
            rows = rows_ref[...]
            gate = dot_nt(rows, gate_ref[...])
            up = dot_nt(rows, up_ref[...])
            size = gate_ref.shape[0]
            hidden_ref[:, i * size : (i + 1) * size] = (
                gate / (1.0 + jnp.exp(-gate)) * up
            ).astype(BF16)

    for q in range(QUARTERS):

        @pl.when(step == gate_steps + q)
        def _():
            result = dot(hidden_ref[...], down_ref[...]).astype(BF16)
            out_ref[:, q * HEAD : (q + 1) * HEAD, :] = result[0:heads].reshape(sources, HEAD, width)
            part = dot(spread(q), result[heads:])
            if q == 0:
                rest_ref[...] = part
            elif q < QUARTERS - 1:
                rest_ref[...] += part
            else:
                out_ref[:, QUARTERS * HEAD :, :] = (
                    (rest_ref[...] + part).astype(BF16).reshape(sources, HEAD, width)
                )


def mix_kernel(back_ref, tok_ref, ids_ref, weight_ref, gain_ref, shift_ref, out_ref, sum_ref):
    experts, _, width = back_ref.shape
    count, model_width = tok_ref.shape
    expert = iota((count, experts), 1)
    first, last = ids_ref[:, 0:1] == expert, ids_ref[:, 1:2] == expert
    hit = jnp.where(first | last, 1.0, 0.0)
    before = flag(iota((count, count), 1) < iota((count, count), 0))
    place = hit * (dot(before, hit.astype(BF16)) + 1.0)
    weight = jnp.where(first, weight_ref[:, 0:1], 0.0) + jnp.where(last, weight_ref[:, 1:2], 0.0)
    high = weight.astype(BF16)
    low = (weight - high.astype(F32)).astype(BF16)
    slots = experts * HEAD
    spread = flag(iota((experts, slots), 1) // HEAD == iota((experts, slots), 0))
    place = dot(place.astype(BF16), spread)
    high, low = dot(high, spread), dot(low, spread)
    column = iota((count, slots), 1)
    in_block = column % HEAD

    def chosen(condition):
        return (
            jnp.where(condition, high, 0.0).astype(BF16),
            jnp.where(condition, low, 0.0).astype(BF16),
        )

    head_high, head_low = chosen(place == (in_block + 1).astype(F32))
    second = place == (HEAD + 1 + column % REST).astype(F32)
    rest = back_ref[:, QUARTERS * HEAD :, :].reshape(slots, width)
    total = jnp.zeros((count, 1), F32)
    for q in range(QUARTERS):
        cols = slice(q * width, (q + 1) * width)
        head = back_ref[:, q * HEAD : (q + 1) * HEAD, :].reshape(slots, width)
        rest_high, rest_low = chosen(second & (in_block // REST == q))
        mixture = dot(head_high, head) + dot(rest_high, rest)
        mixture += dot(head_low, head) + dot(rest_low, rest)
        residual = residual_scale * tok_ref[:, cols].astype(F32) + mixture
        sum_ref[:, cols] = residual
        total += jnp.sum(residual, axis=-1, keepdims=True)
    center = sum_ref[...] - total / model_width
    variance = jnp.mean(center * center, axis=-1, keepdims=True)
    out_ref[...] = (center * lax.rsqrt(variance + norm_eps) * gain_ref[...] + shift_ref[...]).astype(BF16)


def body(tokens, expert_ids, group_weight, expert_share, gate_w, up_w, down_w, out_gain, out_shift):
    tok_count, model_width = tokens.shape
    ep_size = lax.axis_size("ep")
    width = model_width // QUARTERS
    block = (HEAD + REST) * QUARTERS
    hidden = gate_w.shape[1] * lax.axis_size("tp")
    gate, up, down = (
        lax.all_gather(w[0], "tp", axis=0, tiled=True) for w in (gate_w, up_w, down_w)
    )
    buffer = jax.ShapeDtypeStruct((ep_size, block, width), BF16)
    send = pl.pallas_call(
        pack_kernel,
        out_shape=buffer,
        name="pack",
    )(tokens, expert_ids.T)
    received = lax.all_to_all(send, "ep", split_axis=0, concat_axis=0, tiled=True)
    gate_steps = 2
    rows = ep_size * (HEAD + REST)
    results = pl.pallas_call(
        functools.partial(ffn_kernel, gate_steps),
        out_shape=buffer,
        grid=(gate_steps + QUARTERS,),
        in_specs=[
            pl.BlockSpec((ep_size, block, width), lambda i: (0, 0, 0)),
            pl.BlockSpec((hidden // gate_steps, model_width), lambda i: (jnp.minimum(i, gate_steps - 1), 0)),
            pl.BlockSpec((hidden // gate_steps, model_width), lambda i: (jnp.minimum(i, gate_steps - 1), 0)),
            pl.BlockSpec((hidden, width), lambda i: (0, jnp.maximum(i - gate_steps, 0))),
        ],
        out_specs=pl.BlockSpec((ep_size, block, width), lambda i: (0, 0, 0)),
        scratch_shapes=[
            pltpu.VMEM((rows, model_width), BF16),
            pltpu.VMEM((rows, hidden), BF16),
            pltpu.VMEM((ep_size * HEAD, width), F32),
        ],
        name="ffn",
    )(received, gate, up, down)
    back = lax.all_to_all(results, "ep", split_axis=0, concat_axis=0, tiled=True)
    share_norm = expert_share / jnp.sum(expert_share, axis=1, keepdims=True)
    route_weight = group_weight[:, None] * share_norm
    return pl.pallas_call(
        mix_kernel,
        out_shape=jax.ShapeDtypeStruct((tok_count, model_width), BF16),
        scratch_shapes=[pltpu.VMEM((tok_count, model_width), F32)],
        name="mix",
    )(back, tokens, expert_ids, route_weight, out_gain[None], out_shift[None])


def solution(mesh):
    placed = (
        P(("ep", "tp"), None),
        P(("ep", "tp"), None),
        P(("ep", "tp")),
        P(("ep", "tp"), None),
        P("ep", "tp", None),
        P("ep", "tp", None),
        P("ep", "tp", None),
        P(),
        P(),
    )
    return jax.shard_map(
        body, mesh=mesh, in_specs=placed, out_specs=P(("ep", "tp"), None), check_vma=False
    )
```

```python
import functools

import jax
import jax.numpy as jnp
from jax import lax
from jax.experimental import pallas as pl
from jax.experimental.pallas import tpu as pltpu
from jax.sharding import PartitionSpec as P

TOP = 2
residual_scale = 2.0**0.5
norm_eps = 1e-05
BF16 = jnp.bfloat16
F32 = jnp.float32
HEAD = 8
REST = 2
QUARTERS = 4
SLICE = 32
ROOM = 52 * 2**20


def dot(a, b):
    return jnp.dot(a, b, preferred_element_type=F32)


def dot_nt(a, b):
    return lax.dot_general(a, b, (((1,), (1,)), ((), ())), preferred_element_type=F32)


def iota(shape, dim):
    return lax.broadcasted_iota(jnp.int32, shape, dim)


def flag(condition):
    return jnp.where(condition, 1.0, 0.0).astype(BF16)


def send_out(staged_ref, out_ref, sems, j):
    rows = pl.ds(j * HEAD, HEAD)
    copy = pltpu.make_async_copy(staged_ref.at[j], out_ref.at[:, rows, :], sems.at[j])
    copy.start()
    return copy


def pack_kernel(tok_ref, ids_ref, out_ref, staged_ref, sems):
    experts, _, width = out_ref.shape
    count = tok_ref.shape[0]
    expert = iota((experts, count), 0)
    named = (ids_ref[0:1, :] == expert) | (ids_ref[1:2, :] == expert)
    hit = jnp.where(named, 1.0, 0.0)
    before = flag(iota((count, count), 0) < iota((count, count), 1))
    place = hit * (dot(hit.astype(BF16), before) + 1.0)
    slots = experts * HEAD
    spread = flag(iota((slots, experts), 0) // HEAD == iota((slots, experts), 1))
    place = dot(spread, place.astype(BF16))
    row = iota((slots, count), 0)
    in_block = row % HEAD
    head = flag(place == (in_block + 1).astype(F32))
    second = place == (HEAD + 1 + row % REST).astype(F32)
    rest = jnp.zeros((slots, width), F32)
    copies = []
    for q in range(QUARTERS):
        part = tok_ref[:, q * width : (q + 1) * width]
        staged_ref[q] = dot(head, part).astype(BF16).reshape(experts, HEAD, width)
        copies.append(send_out(staged_ref, out_ref, sems, q))
        rest += dot(flag(second & (in_block // REST == q)), part)
    staged_ref[QUARTERS] = rest.astype(BF16).reshape(experts, HEAD, width)
    copies.append(send_out(staged_ref, out_ref, sems, QUARTERS))
    for copy in copies:
        copy.wait()


def ffn_kernel(chunks, recv_ref, *refs):
    pieces, (out_ref, gate_ref, up_ref, down_ref, rows_ref, hidden_ref, staged_ref, sems, out_sems) = (
        refs[:-9],
        refs[-9:],
    )
    sources, _, width = recv_ref.shape
    heads, rests = sources * HEAD, sources * REST
    hidden = gate_ref.shape[0]

    waits = []
    for piece in pieces:
        for base in range(0, piece.shape[0], 3 * SLICE):
            at = len(waits)
            copies = [
                pltpu.make_async_copy(
                    piece.at[pl.ds(base + j * SLICE, SLICE), :],
                    weight.at[pl.ds(at * SLICE, SLICE), :],
                    sems.at[at, j],
                )
                for j, weight in enumerate((gate_ref, up_ref, down_ref))
            ]
            copies[0].start()
            copies[1].start()
            waits.append(copies)
    for copies in waits:
        copies[2].start()

    def pick(q):
        a = iota((rests, heads), 0)
        return flag(iota((rests, heads), 1) == (a // REST) * HEAD + q * REST + a % REST)

    def spread(q):
        a = iota((heads, rests), 1)
        return flag(iota((heads, rests), 0) == (a // REST) * HEAD + q * REST + a % REST)

    rest = recv_ref[:, QUARTERS * HEAD :, :].reshape(heads, width)
    for q in range(QUARTERS):
        cols = slice(q * width, (q + 1) * width)
        rows_ref[0:heads, cols] = recv_ref[:, q * HEAD : (q + 1) * HEAD, :].reshape(heads, width)
        rows_ref[heads:, cols] = dot(pick(q), rest).astype(BF16)

    size = hidden // chunks
    for i in range(chunks):
        for copies in waits[i * size // SLICE : (i + 1) * size // SLICE]:
            copies[0].wait()
            copies[1].wait()
        part = slice(i * size, (i + 1) * size)
        gate = dot_nt(rows_ref[...], gate_ref[part, :])
        up = dot_nt(rows_ref[...], up_ref[part, :])
        hidden_ref[:, part] = (gate / (1.0 + jnp.exp(-gate)) * up).astype(BF16)

    for copies in waits:
        copies[2].wait()
    rest = jnp.zeros((heads, width), F32)
    sent = []
    for q in range(QUARTERS):
        result = dot(hidden_ref[...], down_ref[:, q * width : (q + 1) * width]).astype(BF16)
        staged_ref[q] = result[0:heads].reshape(sources, HEAD, width)
        sent.append(send_out(staged_ref, out_ref, out_sems, q))
        rest += dot(spread(q), result[heads:])
    staged_ref[QUARTERS] = rest.astype(BF16).reshape(sources, HEAD, width)
    sent.append(send_out(staged_ref, out_ref, out_sems, QUARTERS))
    for copy in sent:
        copy.wait()


def mix_kernel(back_ref, tok_ref, ids_ref, weight_ref, gain_ref, shift_ref, out_ref, sum_ref):
    experts, _, width = back_ref.shape
    count, model_width = tok_ref.shape
    expert = iota((count, experts), 1)
    first, last = ids_ref[:, 0:1] == expert, ids_ref[:, 1:2] == expert
    hit = jnp.where(first | last, 1.0, 0.0)
    before = flag(iota((count, count), 1) < iota((count, count), 0))
    place = hit * (dot(before, hit.astype(BF16)) + 1.0)
    weight = jnp.where(first, weight_ref[:, 0:1], 0.0) + jnp.where(last, weight_ref[:, 1:2], 0.0)
    high = weight.astype(BF16)
    low = (weight - high.astype(F32)).astype(BF16)
    slots = experts * HEAD
    spread = flag(iota((experts, slots), 1) // HEAD == iota((experts, slots), 0))
    place = dot(place.astype(BF16), spread)
    high, low = dot(high, spread), dot(low, spread)
    column = iota((count, slots), 1)
    in_block = column % HEAD

    def chosen(condition):
        return (
            jnp.where(condition, high, 0.0).astype(BF16),
            jnp.where(condition, low, 0.0).astype(BF16),
        )

    head_high, head_low = chosen(place == (in_block + 1).astype(F32))
    second = place == (HEAD + 1 + column % REST).astype(F32)
    rest = back_ref[:, QUARTERS * HEAD :, :].reshape(slots, width)
    total = jnp.zeros((count, 1), F32)
    for q in range(QUARTERS):
        cols = slice(q * width, (q + 1) * width)
        head = back_ref[:, q * HEAD : (q + 1) * HEAD, :].reshape(slots, width)
        rest_high, rest_low = chosen(second & (in_block // REST == q))
        mixture = dot(head_high, head) + dot(rest_high, rest)
        mixture += dot(head_low, head) + dot(rest_low, rest)
        residual = residual_scale * tok_ref[:, cols].astype(F32) + mixture
        sum_ref[:, cols] = residual
        total += jnp.sum(residual, axis=-1, keepdims=True)
    center = sum_ref[...] - total / model_width
    variance = jnp.mean(center * center, axis=-1, keepdims=True)
    out_ref[...] = (center * lax.rsqrt(variance + norm_eps) * gain_ref[...] + shift_ref[...]).astype(BF16)


def gather_slices(own):
    size = lax.axis_size("tp")
    partner = [(i, i ^ 1) for i in range(size)]
    onward = [(i, (i + 2 - 4 * (i % 2)) % size) for i in range(size)]
    other = lax.ppermute(own, "tp", partner)
    pieces = [own, other]
    moving = jnp.concatenate([own, other], axis=0)
    steps = size // 4
    for step in range(steps):
        if step == steps - 1:
            moving = moving[: own.shape[0]]
        moving = lax.ppermute(moving, "tp", onward)
        pieces += [moving, lax.ppermute(moving, "tp", partner)]
    return pieces


def body(tokens, expert_ids, group_weight, expert_share, gate_w, up_w, down_w, out_gain, out_shift):
    tok_count, model_width = tokens.shape
    ep_size = lax.axis_size("ep")
    width = model_width // QUARTERS
    block = (HEAD + REST) * QUARTERS
    hidden = gate_w.shape[1] * lax.axis_size("tp")
    buffer = jax.ShapeDtypeStruct((ep_size, block, width), BF16)
    vmem = pl.BlockSpec(memory_space=pltpu.VMEM)
    hbm = pl.BlockSpec(memory_space=pltpu.HBM)
    staged = pltpu.VMEM((QUARTERS + 1, ep_size, HEAD, width), BF16)
    staged_sems = pltpu.SemaphoreType.DMA((QUARTERS + 1,))
    limit = pltpu.CompilerParams(vmem_limit_bytes=32 * 2**20)
    send = pl.pallas_call(
        pack_kernel,
        out_shape=buffer,
        out_specs=hbm,
        scratch_shapes=[staged, staged_sems],
        name="pack",
    )(tokens, expert_ids.T)
    received = lax.all_to_all(send, "ep", split_axis=0, concat_axis=0, tiled=True)
    own = jnp.concatenate([gate_w[0], up_w[0], down_w[0]], axis=0)
    pieces = gather_slices(own)
    rows = ep_size * (HEAD + REST)
    results = pl.pallas_call(
        functools.partial(ffn_kernel, 2),
        out_shape=buffer,
        in_specs=[vmem] + [hbm] * len(pieces),
        out_specs=hbm,
        scratch_shapes=[pltpu.VMEM((hidden, model_width), BF16)] * 3
        + [
            pltpu.VMEM((rows, model_width), BF16),
            pltpu.VMEM((rows, hidden), BF16),
            staged,
            pltpu.SemaphoreType.DMA((hidden // SLICE, 3)),
            staged_sems,
        ],
        compiler_params=pltpu.CompilerParams(vmem_limit_bytes=ROOM),
        name="ffn",
    )(received, *pieces)
    back = lax.all_to_all(results, "ep", split_axis=0, concat_axis=0, tiled=True)
    share_norm = expert_share / jnp.sum(expert_share, axis=1, keepdims=True)
    route_weight = group_weight[:, None] * share_norm
    return pl.pallas_call(
        mix_kernel,
        out_shape=jax.ShapeDtypeStruct((tok_count, model_width), BF16),
        in_specs=[vmem] * 6,
        out_specs=vmem,
        scratch_shapes=[pltpu.VMEM((tok_count, model_width), F32)],
        compiler_params=limit,
        name="mix",
    )(back, tokens, expert_ids, route_weight, out_gain[None], out_shift[None])


def solution(mesh):
    placed = (
        P(("ep", "tp"), None),
        P(("ep", "tp"), None),
        P(("ep", "tp")),
        P(("ep", "tp"), None),
        P("ep", "tp", None),
        P("ep", "tp", None),
        P("ep", "tp", None),
        P(),
        P(),
    )
    return jax.shard_map(
        body, mesh=mesh, in_specs=placed, out_specs=P(("ep", "tp"), None), check_vma=False
    )
```

```python
import functools

import jax
import jax.numpy as jnp
from jax import lax
from jax.experimental import pallas as pl
from jax.experimental.pallas import tpu as pltpu
from jax.sharding import PartitionSpec as P

TOP = 2
residual_scale = 2.0**0.5
norm_eps = 1e-05
BF16 = jnp.bfloat16
F32 = jnp.float32
HEAD = 8
REST = 2
QUARTERS = 4
SLICE = 32
ROOM = 50 * 2**20


def dot(a, b):
    return jnp.dot(a, b, preferred_element_type=F32)


def dot_nt(a, b):
    return lax.dot_general(a, b, (((1,), (1,)), ((), ())), preferred_element_type=F32)


def iota(shape, dim):
    return lax.broadcasted_iota(jnp.int32, shape, dim)


def flag(condition):
    return jnp.where(condition, 1.0, 0.0).astype(BF16)


def send_out(staged_ref, out_ref, sems, j):
    rows = pl.ds(j * HEAD, HEAD)
    copy = pltpu.make_async_copy(staged_ref.at[j], out_ref.at[:, rows, :], sems.at[j])
    copy.start()
    return copy


def pack_kernel(tok_ref, ids_ref, out_ref, staged_ref, sems):
    experts, _, width = out_ref.shape
    count = tok_ref.shape[0]
    expert = iota((experts, count), 0)
    named = (ids_ref[0:1, :] == expert) | (ids_ref[1:2, :] == expert)
    hit = jnp.where(named, 1.0, 0.0)
    before = flag(iota((count, count), 0) < iota((count, count), 1))
    place = hit * (dot(hit.astype(BF16), before) + 1.0)
    slots = experts * HEAD
    spread = flag(iota((slots, experts), 0) // HEAD == iota((slots, experts), 1))
    place = dot(spread, place.astype(BF16))
    row = iota((slots, count), 0)
    in_block = row % HEAD
    head = flag(place == (in_block + 1).astype(F32))
    second = place == (HEAD + 1 + row % REST).astype(F32)
    rest = jnp.zeros((slots, width), F32)
    copies = []
    for q in range(QUARTERS):
        part = tok_ref[:, q * width : (q + 1) * width]
        staged_ref[q] = dot(head, part).astype(BF16).reshape(experts, HEAD, width)
        copies.append(send_out(staged_ref, out_ref, sems, q))
        rest += dot(flag(second & (in_block // REST == q)), part)
    staged_ref[QUARTERS] = rest.astype(BF16).reshape(experts, HEAD, width)
    copies.append(send_out(staged_ref, out_ref, sems, QUARTERS))
    for copy in copies:
        copy.wait()


def ffn_kernel(
    chunks, recv_ref, gathered_ref, _, out_ref, weight_ref, rows_ref, hidden_ref, staged_ref, sems, out_sems
):
    sources, _, width = recv_ref.shape
    heads, rests = sources * HEAD, sources * REST
    slices, _, _, model_width = weight_ref.shape
    size = slices // chunks
    waits = []
    for i in range(chunks):
        part = pl.ds(i * size, size)
        waits.append(pltpu.make_async_copy(gathered_ref.at[part], weight_ref.at[part], sems.at[i]))
        waits[i].start()

    def pick(q):
        a = iota((rests, heads), 0)
        return flag(iota((rests, heads), 1) == (a // REST) * HEAD + q * REST + a % REST)

    def spread(q):
        a = iota((heads, rests), 1)
        return flag(iota((heads, rests), 0) == (a // REST) * HEAD + q * REST + a % REST)

    rest = recv_ref[:, QUARTERS * HEAD :, :].reshape(heads, width)
    for q in range(QUARTERS):
        cols = slice(q * width, (q + 1) * width)
        rows_ref[0:heads, cols] = recv_ref[:, q * HEAD : (q + 1) * HEAD, :].reshape(heads, width)
        rows_ref[heads:, cols] = dot(pick(q), rest).astype(BF16)

    for i in range(chunks):
        waits[i].wait()
        part = slice(i * size, (i + 1) * size)
        gate = dot_nt(rows_ref[...], weight_ref[part, 0].reshape(-1, model_width))
        up = dot_nt(rows_ref[...], weight_ref[part, 1].reshape(-1, model_width))
        hidden_ref[:, i * size * SLICE : (i + 1) * size * SLICE] = (
            gate / (1.0 + jnp.exp(-gate)) * up
        ).astype(BF16)

    rest = jnp.zeros((heads, width), F32)
    sent = []
    for q in range(QUARTERS):
        down = weight_ref[:, 2, :, q * width : (q + 1) * width].reshape(-1, width)
        result = dot(hidden_ref[...], down).astype(BF16)
        staged_ref[q] = result[0:heads].reshape(sources, HEAD, width)
        sent.append(send_out(staged_ref, out_ref, out_sems, q))
        rest += dot(spread(q), result[heads:])
    staged_ref[QUARTERS] = rest.astype(BF16).reshape(sources, HEAD, width)
    sent.append(send_out(staged_ref, out_ref, out_sems, QUARTERS))
    for copy in sent:
        copy.wait()


def mix_kernel(back_ref, tok_ref, ids_ref, weight_ref, gain_ref, shift_ref, out_ref, sum_ref):
    experts, _, width = back_ref.shape
    count, model_width = tok_ref.shape
    expert = iota((count, experts), 1)
    first, last = ids_ref[:, 0:1] == expert, ids_ref[:, 1:2] == expert
    hit = jnp.where(first | last, 1.0, 0.0)
    before = flag(iota((count, count), 1) < iota((count, count), 0))
    place = hit * (dot(before, hit.astype(BF16)) + 1.0)
    weight = jnp.where(first, weight_ref[:, 0:1], 0.0) + jnp.where(last, weight_ref[:, 1:2], 0.0)
    high = weight.astype(BF16)
    low = (weight - high.astype(F32)).astype(BF16)
    slots = experts * HEAD
    spread = flag(iota((experts, slots), 1) // HEAD == iota((experts, slots), 0))
    place = dot(place.astype(BF16), spread)
    high, low = dot(high, spread), dot(low, spread)
    column = iota((count, slots), 1)
    in_block = column % HEAD

    def chosen(condition):
        return (
            jnp.where(condition, high, 0.0).astype(BF16),
            jnp.where(condition, low, 0.0).astype(BF16),
        )

    head_high, head_low = chosen(place == (in_block + 1).astype(F32))
    second = place == (HEAD + 1 + column % REST).astype(F32)
    rest = back_ref[:, QUARTERS * HEAD :, :].reshape(slots, width)
    total = jnp.zeros((count, 1), F32)
    for q in range(QUARTERS):
        cols = slice(q * width, (q + 1) * width)
        head = back_ref[:, q * HEAD : (q + 1) * HEAD, :].reshape(slots, width)
        rest_high, rest_low = chosen(second & (in_block // REST == q))
        mixture = dot(head_high, head) + dot(rest_high, rest)
        mixture += dot(head_low, head) + dot(rest_low, rest)
        residual = residual_scale * tok_ref[:, cols].astype(F32) + mixture
        sum_ref[:, cols] = residual
        total += jnp.sum(residual, axis=-1, keepdims=True)
    center = sum_ref[...] - total / model_width
    variance = jnp.mean(center * center, axis=-1, keepdims=True)
    out_ref[...] = (center * lax.rsqrt(variance + norm_eps) * gain_ref[...] + shift_ref[...]).astype(BF16)


def gather_slices(own):
    size = lax.axis_size("tp")
    partner = [(i, i ^ 1) for i in range(size)]
    onward = [(i, (i + 2 - 4 * (i % 2)) % size) for i in range(size)]
    other = lax.ppermute(own, "tp", partner)
    pieces = [own, other]
    chains = [own, other]
    steps = size // 4
    for step in range(steps):
        if step == steps - 1:
            chains = chains[:1]
        chains = [lax.ppermute(c, "tp", onward) for c in chains]
        pieces += chains
        pieces += [lax.ppermute(c, "tp", partner) for c in chains]
    return jnp.concatenate(pieces, axis=0)


def body(tokens, expert_ids, group_weight, expert_share, gate_w, up_w, down_w, out_gain, out_shift):
    tok_count, model_width = tokens.shape
    ep_size = lax.axis_size("ep")
    width = model_width // QUARTERS
    block = (HEAD + REST) * QUARTERS
    hidden = gate_w.shape[1] * lax.axis_size("tp")
    buffer = jax.ShapeDtypeStruct((ep_size, block, width), BF16)
    vmem = pl.BlockSpec(memory_space=pltpu.VMEM)
    hbm = pl.BlockSpec(memory_space=pl.ANY)
    staged = pltpu.VMEM((QUARTERS + 1, ep_size, HEAD, width), BF16)
    staged_sems = pltpu.SemaphoreType.DMA((QUARTERS + 1,))
    limit = pltpu.CompilerParams(vmem_limit_bytes=32 * 2**20)
    send = pl.pallas_call(
        pack_kernel,
        out_shape=buffer,
        out_specs=hbm,
        scratch_shapes=[staged, staged_sems],
        name="pack",
    )(tokens, expert_ids.T)
    received = lax.all_to_all(send, "ep", split_axis=0, concat_axis=0, tiled=True)
    own = jnp.concatenate([gate_w[0], up_w[0], down_w[0]], axis=0)
    gathered = gather_slices(own).reshape(-1, 3, SLICE, model_width)
    rows = ep_size * (HEAD + REST)
    results = pl.pallas_call(
        functools.partial(ffn_kernel, 2),
        out_shape=buffer,
        in_specs=[vmem, hbm, hbm],
        out_specs=hbm,
        scratch_shapes=[
            pltpu.VMEM(gathered.shape, BF16),
            pltpu.VMEM((rows, model_width), BF16),
            pltpu.VMEM((rows, hidden), BF16),
            staged,
            pltpu.SemaphoreType.DMA((2,)),
            staged_sems,
        ],
        input_output_aliases={2: 0},
        compiler_params=pltpu.CompilerParams(vmem_limit_bytes=ROOM),
        name="ffn",
    )(received, gathered, send)
    back = lax.all_to_all(results, "ep", split_axis=0, concat_axis=0, tiled=True)
    share_norm = expert_share / jnp.sum(expert_share, axis=1, keepdims=True)
    route_weight = group_weight[:, None] * share_norm
    return pl.pallas_call(
        mix_kernel,
        out_shape=jax.ShapeDtypeStruct((tok_count, model_width), BF16),
        in_specs=[vmem] * 6,
        out_specs=vmem,
        scratch_shapes=[pltpu.VMEM((tok_count, model_width), F32)],
        compiler_params=limit,
        name="mix",
    )(back, tokens, expert_ids, route_weight, out_gain[None], out_shift[None])


def solution(mesh):
    placed = (
        P(("ep", "tp"), None),
        P(("ep", "tp"), None),
        P(("ep", "tp")),
        P(("ep", "tp"), None),
        P("ep", "tp", None),
        P("ep", "tp", None),
        P("ep", "tp", None),
        P(),
        P(),
    )
    return jax.shard_map(
        body, mesh=mesh, in_specs=placed, out_specs=P(("ep", "tp"), None), check_vma=False
    )
```

```python
import functools

import jax
import jax.numpy as jnp
from jax import lax
from jax.experimental import pallas as pl
from jax.experimental.pallas import tpu as pltpu
from jax.sharding import PartitionSpec as P

TOP = 2
residual_scale = 2.0**0.5
norm_eps = 1e-05
BF16 = jnp.bfloat16
F32 = jnp.float32
HEAD = 8
REST = 2
QUARTERS = 4
SLICE = 32
ROOM = 50 * 2**20
LATE = 1


def dot(a, b):
    return jnp.dot(a, b, preferred_element_type=F32)


def dot_nt(a, b):
    return lax.dot_general(a, b, (((1,), (1,)), ((), ())), preferred_element_type=F32)


def iota(shape, dim):
    return lax.broadcasted_iota(jnp.int32, shape, dim)


def flag(condition):
    return jnp.where(condition, 1.0, 0.0).astype(BF16)


def send_out(staged_ref, out_ref, sems, j):
    rows = pl.ds(j * HEAD, HEAD)
    copy = pltpu.make_async_copy(staged_ref.at[j], out_ref.at[:, rows, :], sems.at[j])
    copy.start()
    return copy


def pack_kernel(tok_ref, ids_ref, out_ref, staged_ref, sems):
    experts, _, width = out_ref.shape
    count = tok_ref.shape[0]
    expert = iota((experts, count), 0)
    named = (ids_ref[0:1, :] == expert) | (ids_ref[1:2, :] == expert)
    hit = jnp.where(named, 1.0, 0.0)
    before = flag(iota((count, count), 0) < iota((count, count), 1))
    place = hit * (dot(hit.astype(BF16), before) + 1.0)
    slots = experts * HEAD
    spread = flag(iota((slots, experts), 0) // HEAD == iota((slots, experts), 1))
    place = dot(spread, place.astype(BF16))
    row = iota((slots, count), 0)
    in_block = row % HEAD
    head = flag(place == (in_block + 1).astype(F32))
    second = place == (HEAD + 1 + row % REST).astype(F32)
    rest = jnp.zeros((slots, width), F32)
    copies = []
    for q in range(QUARTERS):
        part = tok_ref[:, q * width : (q + 1) * width]
        staged_ref[q] = dot(head, part).astype(BF16).reshape(experts, HEAD, width)
        copies.append(send_out(staged_ref, out_ref, sems, q))
        rest += dot(flag(second & (in_block // REST == q)), part)
    staged_ref[QUARTERS] = rest.astype(BF16).reshape(experts, HEAD, width)
    copies.append(send_out(staged_ref, out_ref, sems, QUARTERS))
    for copy in copies:
        copy.wait()


def ffn_kernel(
    chunks, recv_ref, _, *refs
):
    pieces, (out_ref, weight_ref, rows_ref, hidden_ref, staged_ref, sems, out_sems) = refs[:-7], refs[-7:]
    sources, _, width = recv_ref.shape
    heads, rests = sources * HEAD, sources * REST
    slices, _, _, model_width = weight_ref.shape
    size = slices // chunks
    waits, at = [], 0
    for n, piece in enumerate(pieces):
        copy = pltpu.make_async_copy(piece, weight_ref.at[pl.ds(at, piece.shape[0])], sems.at[n])
        copy.start()
        at += piece.shape[0]
        waits.append((at, copy))

    def pick(q):
        a = iota((rests, heads), 0)
        return flag(iota((rests, heads), 1) == (a // REST) * HEAD + q * REST + a % REST)

    def spread(q):
        a = iota((heads, rests), 1)
        return flag(iota((heads, rests), 0) == (a // REST) * HEAD + q * REST + a % REST)

    rest = recv_ref[:, QUARTERS * HEAD :, :].reshape(heads, width)
    for q in range(QUARTERS):
        cols = slice(q * width, (q + 1) * width)
        rows_ref[0:heads, cols] = recv_ref[:, q * HEAD : (q + 1) * HEAD, :].reshape(heads, width)
        rows_ref[heads:, cols] = dot(pick(q), rest).astype(BF16)

    for i in range(chunks):
        for end, copy in waits:
            if i * size < end <= (i + 1) * size:
                copy.wait()
        part = slice(i * size, (i + 1) * size)
        gate = dot_nt(rows_ref[...], weight_ref[part, 0].reshape(-1, model_width))
        up = dot_nt(rows_ref[...], weight_ref[part, 1].reshape(-1, model_width))
        hidden_ref[:, i * size * SLICE : (i + 1) * size * SLICE] = (
            gate / (1.0 + jnp.exp(-gate)) * up
        ).astype(BF16)

    rest = jnp.zeros((heads, width), F32)
    sent = []
    for q in range(QUARTERS):
        down = weight_ref[:, 2, :, q * width : (q + 1) * width].reshape(-1, width)
        result = dot(hidden_ref[...], down).astype(BF16)
        staged_ref[q] = result[0:heads].reshape(sources, HEAD, width)
        sent.append(send_out(staged_ref, out_ref, out_sems, q))
        rest += dot(spread(q), result[heads:])
    staged_ref[QUARTERS] = rest.astype(BF16).reshape(sources, HEAD, width)
    sent.append(send_out(staged_ref, out_ref, out_sems, QUARTERS))
    for copy in sent:
        copy.wait()


def collect_kernel(late_ref, own_ref, *refs):
    pieces, (out_ref, staged_ref, in_sems, out_sems) = refs[:-4], refs[-4:]
    half = len(pieces) // 2

    def load(piece, n):
        return pltpu.make_async_copy(piece, staged_ref.at[n], in_sems.at[n])

    def store(n):
        return pltpu.make_async_copy(staged_ref.at[n], out_ref.at[n], out_sems.at[n])

    load(own_ref, 0).start()
    for late, chosen in ((0, pieces[:half]), (1, pieces[half:])):

        @pl.when(late_ref[0] == late)
        def _():
            for n, piece in enumerate(chosen):
                load(piece, n + 1).start()

    for n in range(half + 1):
        load(own_ref, n).wait()
        store(n).start()
    for n in range(half + 1):
        store(n).wait()


def mix_kernel(back_ref, tok_ref, ids_ref, weight_ref, gain_ref, shift_ref, out_ref, sum_ref):
    experts, _, width = back_ref.shape
    count, model_width = tok_ref.shape
    expert = iota((count, experts), 1)
    first, last = ids_ref[:, 0:1] == expert, ids_ref[:, 1:2] == expert
    hit = jnp.where(first | last, 1.0, 0.0)
    before = flag(iota((count, count), 1) < iota((count, count), 0))
    place = hit * (dot(before, hit.astype(BF16)) + 1.0)
    weight = jnp.where(first, weight_ref[:, 0:1], 0.0) + jnp.where(last, weight_ref[:, 1:2], 0.0)
    high = weight.astype(BF16)
    low = (weight - high.astype(F32)).astype(BF16)
    slots = experts * HEAD
    spread = flag(iota((experts, slots), 1) // HEAD == iota((experts, slots), 0))
    place = dot(place.astype(BF16), spread)
    high, low = dot(high, spread), dot(low, spread)
    column = iota((count, slots), 1)
    in_block = column % HEAD

    def chosen(condition):
        return (
            jnp.where(condition, high, 0.0).astype(BF16),
            jnp.where(condition, low, 0.0).astype(BF16),
        )

    head_high, head_low = chosen(place == (in_block + 1).astype(F32))
    second = place == (HEAD + 1 + column % REST).astype(F32)
    rest = back_ref[:, QUARTERS * HEAD :, :].reshape(slots, width)
    total = jnp.zeros((count, 1), F32)
    for q in range(QUARTERS):
        cols = slice(q * width, (q + 1) * width)
        head = back_ref[:, q * HEAD : (q + 1) * HEAD, :].reshape(slots, width)
        rest_high, rest_low = chosen(second & (in_block // REST == q))
        mixture = dot(head_high, head) + dot(rest_high, rest)
        mixture += dot(head_low, head) + dot(rest_low, rest)
        residual = residual_scale * tok_ref[:, cols].astype(F32) + mixture
        sum_ref[:, cols] = residual
        total += jnp.sum(residual, axis=-1, keepdims=True)
    center = sum_ref[...] - total / model_width
    variance = jnp.mean(center * center, axis=-1, keepdims=True)
    out_ref[...] = (center * lax.rsqrt(variance + norm_eps) * gain_ref[...] + shift_ref[...]).astype(BF16)


def ring(own, core):
    size = lax.axis_size("tp")

    def move(x, chips):
        return lax.ppermute(x, "tp", [(i, (i + 2 * chips) % size) for i in range(core, size, 2)])

    up, down = move(own, 2), move(own, -2)
    return [up, down, move(own, 1), move(own, -1), move(up, 2), move(up, 1), move(down, -1)]


def body(tokens, expert_ids, group_weight, expert_share, gate_w, up_w, down_w, out_gain, out_shift):
    tok_count, model_width = tokens.shape
    ep_size = lax.axis_size("ep")
    width = model_width // QUARTERS
    block = (HEAD + REST) * QUARTERS
    hidden = gate_w.shape[1] * lax.axis_size("tp")
    buffer = jax.ShapeDtypeStruct((ep_size, block, width), BF16)
    vmem = pl.BlockSpec(memory_space=pltpu.VMEM)
    hbm = pl.BlockSpec(memory_space=pl.ANY)
    staged = pltpu.VMEM((QUARTERS + 1, ep_size, HEAD, width), BF16)
    staged_sems = pltpu.SemaphoreType.DMA((QUARTERS + 1,))
    limit = pltpu.CompilerParams(vmem_limit_bytes=32 * 2**20)
    send = pl.pallas_call(
        pack_kernel,
        out_shape=buffer,
        out_specs=hbm,
        scratch_shapes=[staged, staged_sems],
        name="pack",
    )(tokens, expert_ids.T)
    late = (lax.axis_index("tp") % 2 == LATE).astype(jnp.int32).reshape(1)
    own = jnp.concatenate([gate_w[0], up_w[0], down_w[0]], axis=0)
    late_pieces = ring(own, LATE)
    smem = pl.BlockSpec(memory_space=pltpu.SMEM)
    send, late_pieces = lax.optimization_barrier((send, late_pieces))
    received = lax.all_to_all(send, "ep", split_axis=0, concat_axis=0, tiled=True)
    own, send = lax.optimization_barrier((own, send))
    early_pieces = ring(own, 1 - LATE)
    count = len(early_pieces) + 1
    slices = (count,) + own.shape
    collected = pl.pallas_call(
        collect_kernel,
        out_shape=jax.ShapeDtypeStruct(slices, BF16),
        in_specs=[smem] + [hbm] * (2 * count - 1),
        out_specs=hbm,
        scratch_shapes=[
            pltpu.VMEM(slices, BF16),
            pltpu.SemaphoreType.DMA((count,)),
            pltpu.SemaphoreType.DMA((count,)),
        ],
        name="collect",
    )(late, own, *early_pieces, *late_pieces)
    other = lax.ppermute(collected, "tp", [(i, i ^ 1) for i in range(lax.axis_size("tp"))])
    pieces = [p.reshape(count, 3, SLICE, model_width) for p in (collected, other)]
    rows = ep_size * (HEAD + REST)
    results = pl.pallas_call(
        functools.partial(ffn_kernel, 2),
        out_shape=buffer,
        in_specs=[vmem] + [hbm] * (len(pieces) + 1),
        out_specs=hbm,
        scratch_shapes=[
            pltpu.VMEM((hidden // SLICE, 3, SLICE, model_width), BF16),
            pltpu.VMEM((rows, model_width), BF16),
            pltpu.VMEM((rows, hidden), BF16),
            staged,
            pltpu.SemaphoreType.DMA((len(pieces),)),
            staged_sems,
        ],
        input_output_aliases={1: 0},
        compiler_params=pltpu.CompilerParams(vmem_limit_bytes=ROOM),
        name="ffn",
    )(received, send, *pieces)
    back = lax.all_to_all(results, "ep", split_axis=0, concat_axis=0, tiled=True)
    share_norm = expert_share / jnp.sum(expert_share, axis=1, keepdims=True)
    route_weight = group_weight[:, None] * share_norm
    return pl.pallas_call(
        mix_kernel,
        out_shape=jax.ShapeDtypeStruct((tok_count, model_width), BF16),
        in_specs=[vmem] * 6,
        out_specs=vmem,
        scratch_shapes=[pltpu.VMEM((tok_count, model_width), F32)],
        compiler_params=limit,
        name="mix",
    )(back, tokens, expert_ids, route_weight, out_gain[None], out_shift[None])


def solution(mesh):
    placed = (
        P(("ep", "tp"), None),
        P(("ep", "tp"), None),
        P(("ep", "tp")),
        P(("ep", "tp"), None),
        P("ep", "tp", None),
        P("ep", "tp", None),
        P("ep", "tp", None),
        P(),
        P(),
    )
    return jax.shard_map(
        body, mesh=mesh, in_specs=placed, out_specs=P(("ep", "tp"), None), check_vma=False
    )
```

```python
import functools

import jax
import jax.numpy as jnp
from jax import lax
from jax.experimental import pallas as pl
from jax.experimental.pallas import tpu as pltpu
from jax.sharding import PartitionSpec as P


residual_scale = 2.0**0.5
norm_eps = 1e-05
BF16 = jnp.bfloat16
F32 = jnp.float32
HEAD = 8
REST = 2
QUARTERS = 4
SLICE = 32
ROOM = 47 * 2**20
LATE = 1


def dot(a, b):
    return jnp.dot(a, b, preferred_element_type=F32)


def dot_nt(a, b):
    return lax.dot_general(a, b, (((1,), (1,)), ((), ())), preferred_element_type=F32)


def iota(shape, dim):
    return lax.broadcasted_iota(jnp.int32, shape, dim)


def flag(condition):
    return jnp.where(condition, 1.0, 0.0).astype(BF16)


def send_out(staged_ref, out_ref, sems, j):
    rows = pl.ds(j * HEAD, HEAD)
    copy = pltpu.make_async_copy(staged_ref.at[j], out_ref.at[:, rows, :], sems.at[j])
    copy.start()
    return copy


def pack_kernel(tok_ref, ids_ref, out_ref, staged_ref, sems):
    experts, _, width = out_ref.shape
    count = tok_ref.shape[0]
    expert = iota((experts, count), 0)
    named = (ids_ref[0:1, :] == expert) | (ids_ref[1:2, :] == expert)
    hit = jnp.where(named, 1.0, 0.0)
    before = flag(iota((count, count), 0) < iota((count, count), 1))
    place = hit * (dot(hit.astype(BF16), before) + 1.0)
    slots = experts * HEAD
    spread = flag(iota((slots, experts), 0) // HEAD == iota((slots, experts), 1))
    place = dot(spread, place.astype(BF16))
    row = iota((slots, count), 0)
    in_block = row % HEAD
    head = flag(place == (in_block + 1).astype(F32))
    second = place == (HEAD + 1 + row % REST).astype(F32)
    rest = jnp.zeros((slots, width), F32)
    copies = []
    for q in range(QUARTERS):
        part = tok_ref[:, q * width : (q + 1) * width]
        staged_ref[q] = dot(head, part).astype(BF16).reshape(experts, HEAD, width)
        copies.append(send_out(staged_ref, out_ref, sems, q))
        rest += dot(flag(second & (in_block // REST == q)), part)
    staged_ref[QUARTERS] = rest.astype(BF16).reshape(experts, HEAD, width)
    copies.append(send_out(staged_ref, out_ref, sems, QUARTERS))
    for copy in copies:
        copy.wait()


def ffn_kernel(
    chunks, recv_ref, _, *refs
):
    pieces, (out_ref, weight_ref, rows_ref, hidden_ref, staged_ref, sems, out_sems) = refs[:-7], refs[-7:]
    sources, _, width = recv_ref.shape
    heads, rests = sources * HEAD, sources * REST
    slices, _, _, model_width = weight_ref.shape
    size = slices // chunks
    waits, at = [], 0
    for n, piece in enumerate(pieces):
        copy = pltpu.make_async_copy(piece, weight_ref.at[pl.ds(at, piece.shape[0])], sems.at[n])
        copy.start()
        at += piece.shape[0]
        waits.append((at, copy))

    def pick(q):
        a = iota((rests, heads), 0)
        return flag(iota((rests, heads), 1) == (a // REST) * HEAD + q * REST + a % REST)

    def spread(q):
        a = iota((heads, rests), 1)
        return flag(iota((heads, rests), 0) == (a // REST) * HEAD + q * REST + a % REST)

    rest = recv_ref[:, QUARTERS * HEAD :, :].reshape(heads, width)
    for q in range(QUARTERS):
        cols = slice(q * width, (q + 1) * width)
        rows_ref[0:heads, cols] = recv_ref[:, q * HEAD : (q + 1) * HEAD, :].reshape(heads, width)
        rows_ref[heads:, cols] = dot(pick(q), rest).astype(BF16)

    for i in range(chunks):
        for end, copy in waits:
            if i * size < end <= (i + 1) * size:
                copy.wait()
        part = slice(i * size, (i + 1) * size)
        gate = dot_nt(rows_ref[...], weight_ref[part, 0].reshape(-1, model_width))
        up = dot_nt(rows_ref[...], weight_ref[part, 1].reshape(-1, model_width))
        hidden_ref[:, i * size * SLICE : (i + 1) * size * SLICE] = (
            gate / (1.0 + jnp.exp(-gate)) * up
        ).astype(BF16)

    rest = jnp.zeros((heads, width), F32)
    sent = []
    for q in range(QUARTERS):
        down = weight_ref[:, 2, :, q * width : (q + 1) * width].reshape(-1, width)
        result = dot(hidden_ref[...], down).astype(BF16)
        staged_ref[q] = result[0:heads].reshape(sources, HEAD, width)
        sent.append(send_out(staged_ref, out_ref, out_sems, q))
        rest += dot(spread(q), result[heads:])
    staged_ref[QUARTERS] = rest.astype(BF16).reshape(sources, HEAD, width)
    sent.append(send_out(staged_ref, out_ref, out_sems, QUARTERS))
    for copy in sent:
        copy.wait()


def collect_kernel(shared, late_ref, *refs):
    pieces, (out_ref, staged_ref, in_sems, out_sems) = refs[:-4], refs[-4:]
    each = (len(pieces) - shared) // 2
    count = shared + each

    def load(piece, n):
        return pltpu.make_async_copy(piece, staged_ref.at[n], in_sems.at[n])

    def store(n):
        return pltpu.make_async_copy(staged_ref.at[n], out_ref.at[n], out_sems.at[n])

    for n in range(shared):
        load(pieces[n], n).start()
    for late in range(2):

        @pl.when(late_ref[0] == late)
        def _():
            for n in range(each):
                load(pieces[shared + late * each + n], shared + n).start()

    for n in range(count):
        load(pieces[0], n).wait()
        store(n).start()
    for n in range(count):
        store(n).wait()


def mix_kernel(back_ref, tok_ref, ids_ref, weight_ref, gain_ref, shift_ref, out_ref, sum_ref):
    experts, _, width = back_ref.shape
    count, model_width = tok_ref.shape
    expert = iota((count, experts), 1)
    first, last = ids_ref[:, 0:1] == expert, ids_ref[:, 1:2] == expert
    hit = jnp.where(first | last, 1.0, 0.0)
    before = flag(iota((count, count), 1) < iota((count, count), 0))
    place = hit * (dot(before, hit.astype(BF16)) + 1.0)
    weight = jnp.where(first, weight_ref[:, 0:1], 0.0) + jnp.where(last, weight_ref[:, 1:2], 0.0)
    high = weight.astype(BF16)
    low = (weight - high.astype(F32)).astype(BF16)
    slots = experts * HEAD
    spread = flag(iota((experts, slots), 1) // HEAD == iota((experts, slots), 0))
    place = dot(place.astype(BF16), spread)
    high, low = dot(high, spread), dot(low, spread)
    column = iota((count, slots), 1)
    in_block = column % HEAD

    def chosen(condition):
        return (
            jnp.where(condition, high, 0.0).astype(BF16),
            jnp.where(condition, low, 0.0).astype(BF16),
        )

    head_high, head_low = chosen(place == (in_block + 1).astype(F32))
    second = place == (HEAD + 1 + column % REST).astype(F32)
    rest = back_ref[:, QUARTERS * HEAD :, :].reshape(slots, width)
    total = jnp.zeros((count, 1), F32)
    for q in range(QUARTERS):
        cols = slice(q * width, (q + 1) * width)
        head = back_ref[:, q * HEAD : (q + 1) * HEAD, :].reshape(slots, width)
        rest_high, rest_low = chosen(second & (in_block // REST == q))
        mixture = dot(head_high, head) + dot(rest_high, rest)
        mixture += dot(head_low, head) + dot(rest_low, rest)
        residual = residual_scale * tok_ref[:, cols].astype(F32) + mixture
        sum_ref[:, cols] = residual
        total += jnp.sum(residual, axis=-1, keepdims=True)
    center = sum_ref[...] - total / model_width
    variance = jnp.mean(center * center, axis=-1, keepdims=True)
    out_ref[...] = (center * lax.rsqrt(variance + norm_eps) * gain_ref[...] + shift_ref[...]).astype(BF16)


def ring(own, core):
    size = lax.axis_size("tp")

    def move(x, chips):
        return lax.ppermute(x, "tp", [(i, (i + 2 * chips) % size) for i in range(core, size, 2)])

    up, down = move(own, 2), move(own, -2)
    first = [up, down, move(own, 1), move(own, -1)]
    second = []
    for x, chips in ((up, 2), (up, 1), (down, -1)):
        second.append(move(x, chips))
    return first, second


def body(tokens, expert_ids, group_weight, expert_share, gate_w, up_w, down_w, out_gain, out_shift):
    tok_count, model_width = tokens.shape
    ep_size = lax.axis_size("ep")
    width = model_width // QUARTERS
    block = (HEAD + REST) * QUARTERS
    hidden = gate_w.shape[1] * lax.axis_size("tp")
    buffer = jax.ShapeDtypeStruct((ep_size, block, width), BF16)
    vmem = pl.BlockSpec(memory_space=pltpu.VMEM)
    hbm = pl.BlockSpec(memory_space=pl.ANY)
    staged = pltpu.VMEM((QUARTERS + 1, ep_size, HEAD, width), BF16)
    staged_sems = pltpu.SemaphoreType.DMA((QUARTERS + 1,))
    limit = pltpu.CompilerParams(vmem_limit_bytes=32 * 2**20)
    send = pl.pallas_call(
        pack_kernel,
        out_shape=buffer,
        out_specs=hbm,
        scratch_shapes=[staged, staged_sems],
        name="pack",
    )(tokens, expert_ids.T)
    late = (lax.axis_index("tp") % 2 == LATE).astype(jnp.int32).reshape(1)
    own = jnp.concatenate([gate_w[0], up_w[0], down_w[0]], axis=0)
    late_pieces = ring(own, LATE)
    smem = pl.BlockSpec(memory_space=pltpu.SMEM)
    send, late_pieces = lax.optimization_barrier((send, late_pieces))
    received = lax.all_to_all(send, "ep", split_axis=0, concat_axis=0, tiled=True)
    own, send = lax.optimization_barrier((own, send))
    early_pieces = ring(own, 1 - LATE)

    def collect(shared, first, second):
        pieces = shared + first + second
        count = len(shared) + len(first)
        slices = (count,) + own.shape
        mine = pl.pallas_call(
            functools.partial(collect_kernel, len(shared)),
            out_shape=jax.ShapeDtypeStruct(slices, BF16),
            in_specs=[smem] + [hbm] * len(pieces),
            out_specs=hbm,
            scratch_shapes=[
                pltpu.VMEM(slices, BF16),
                pltpu.SemaphoreType.DMA((count,)),
                pltpu.SemaphoreType.DMA((count,)),
            ],
        )(late, *pieces)
        other = lax.ppermute(mine, "tp", [(i, i ^ 1) for i in range(lax.axis_size("tp"))])
        return [x.reshape(count, 3, SLICE, model_width) for x in (mine, other)]

    near = collect([own], early_pieces[0], late_pieces[0])
    far = collect([], early_pieces[1], late_pieces[1])
    pieces = [near[0], far[0], near[1], far[1]]
    rows = ep_size * (HEAD + REST)
    results = pl.pallas_call(
        functools.partial(ffn_kernel, 2),
        out_shape=buffer,
        in_specs=[vmem] + [hbm] * (len(pieces) + 1),
        out_specs=hbm,
        scratch_shapes=[
            pltpu.VMEM((hidden // SLICE, 3, SLICE, model_width), BF16),
            pltpu.VMEM((rows, model_width), BF16),
            pltpu.VMEM((rows, hidden), BF16),
            staged,
            pltpu.SemaphoreType.DMA((len(pieces),)),
            staged_sems,
        ],
        input_output_aliases={1: 0},
        compiler_params=pltpu.CompilerParams(vmem_limit_bytes=ROOM),
        name="ffn",
    )(received, send, *pieces)
    back = lax.all_to_all(results, "ep", split_axis=0, concat_axis=0, tiled=True)
    share_norm = expert_share / jnp.sum(expert_share, axis=1, keepdims=True)
    route_weight = group_weight[:, None] * share_norm
    return pl.pallas_call(
        mix_kernel,
        out_shape=jax.ShapeDtypeStruct((tok_count, model_width), BF16),
        in_specs=[vmem] * 6,
        out_specs=vmem,
        scratch_shapes=[pltpu.VMEM((tok_count, model_width), F32)],
        compiler_params=limit,
        name="mix",
    )(back, tokens, expert_ids, route_weight, out_gain[None], out_shift[None])


def solution(mesh):
    placed = (
        P(("ep", "tp"), None),
        P(("ep", "tp"), None),
        P(("ep", "tp")),
        P(("ep", "tp"), None),
        P("ep", "tp", None),
        P("ep", "tp", None),
        P("ep", "tp", None),
        P(),
        P(),
    )
    return jax.shard_map(
        body, mesh=mesh, in_specs=placed, out_specs=P(("ep", "tp"), None), check_vma=False
    )
```

```python
import functools

import jax
import jax.numpy as jnp
from jax import lax
from jax.experimental import pallas as pl
from jax.experimental.pallas import tpu as pltpu
from jax.sharding import PartitionSpec as P

TOP = 2
residual_scale = 2.0**0.5
norm_eps = 1e-05
BF16 = jnp.bfloat16
F32 = jnp.float32
HEAD = 8
REST = 2
QUARTERS = 4
SLICE = 32
ROOM = 50 * 2**20
LATE = 1
HOLD = 27000


def dot(a, b):
    return jnp.dot(a, b, preferred_element_type=F32)


def dot_nt(a, b):
    return lax.dot_general(a, b, (((1,), (1,)), ((), ())), preferred_element_type=F32)


def iota(shape, dim):
    return lax.broadcasted_iota(jnp.int32, shape, dim)


def flag(condition):
    return jnp.where(condition, 1.0, 0.0).astype(BF16)


def send_out(staged_ref, out_ref, sems, j):
    rows = pl.ds(j * HEAD, HEAD)
    copy = pltpu.make_async_copy(staged_ref.at[j], out_ref.at[:, rows, :], sems.at[j])
    copy.start()
    return copy


def pack_kernel(tok_ref, ids_ref, out_ref, staged_ref, sems):
    experts, _, width = out_ref.shape
    count = tok_ref.shape[0]
    expert = iota((experts, count), 0)
    named = (ids_ref[0:1, :] == expert) | (ids_ref[1:2, :] == expert)
    hit = jnp.where(named, 1.0, 0.0)
    before = flag(iota((count, count), 0) < iota((count, count), 1))
    place = hit * (dot(hit.astype(BF16), before) + 1.0)
    slots = experts * HEAD
    spread = flag(iota((slots, experts), 0) // HEAD == iota((slots, experts), 1))
    place = dot(spread, place.astype(BF16))
    row = iota((slots, count), 0)
    in_block = row % HEAD
    head = flag(place == (in_block + 1).astype(F32))
    second = place == (HEAD + 1 + row % REST).astype(F32)
    rest = jnp.zeros((slots, width), F32)
    copies = []
    for q in range(QUARTERS):
        part = tok_ref[:, q * width : (q + 1) * width]
        staged_ref[q] = dot(head, part).astype(BF16).reshape(experts, HEAD, width)
        copies.append(send_out(staged_ref, out_ref, sems, q))
        rest += dot(flag(second & (in_block // REST == q)), part)
    staged_ref[QUARTERS] = rest.astype(BF16).reshape(experts, HEAD, width)
    copies.append(send_out(staged_ref, out_ref, sems, QUARTERS))
    for copy in copies:
        copy.wait()


def ffn_kernel(
    chunks, recv_ref, _, *refs
):
    pieces, (out_ref, weight_ref, rows_ref, hidden_ref, staged_ref, sems, out_sems) = refs[:-7], refs[-7:]
    sources, _, width = recv_ref.shape
    heads, rests = sources * HEAD, sources * REST
    slices, _, _, model_width = weight_ref.shape
    size = slices // chunks
    waits = []
    for n in range(chunks):
        part = pl.ds(n * size, size)
        copy = pltpu.make_async_copy(pieces[0].at[part], weight_ref.at[part], sems.at[n])
        copy.start()
        waits.append(((n + 1) * size, copy))

    def pick(q):
        a = iota((rests, heads), 0)
        return flag(iota((rests, heads), 1) == (a // REST) * HEAD + q * REST + a % REST)

    def spread(q):
        a = iota((heads, rests), 1)
        return flag(iota((heads, rests), 0) == (a // REST) * HEAD + q * REST + a % REST)

    rest = recv_ref[:, QUARTERS * HEAD :, :].reshape(heads, width)
    for q in range(QUARTERS):
        cols = slice(q * width, (q + 1) * width)
        rows_ref[0:heads, cols] = recv_ref[:, q * HEAD : (q + 1) * HEAD, :].reshape(heads, width)
        rows_ref[heads:, cols] = dot(pick(q), rest).astype(BF16)

    for i in range(chunks):
        for end, copy in waits:
            if i * size < end <= (i + 1) * size:
                copy.wait()
        part = slice(i * size, (i + 1) * size)
        gate = dot_nt(rows_ref[...], weight_ref[part, 0].reshape(-1, model_width))
        up = dot_nt(rows_ref[...], weight_ref[part, 1].reshape(-1, model_width))
        hidden_ref[:, i * size * SLICE : (i + 1) * size * SLICE] = (
            gate / (1.0 + jnp.exp(-gate)) * up
        ).astype(BF16)

    rest = jnp.zeros((heads, width), F32)
    sent = []
    for q in range(QUARTERS):
        down = weight_ref[:, 2, :, q * width : (q + 1) * width].reshape(-1, width)
        result = dot(hidden_ref[...], down).astype(BF16)
        staged_ref[q] = result[0:heads].reshape(sources, HEAD, width)
        sent.append(send_out(staged_ref, out_ref, out_sems, q))
        rest += dot(spread(q), result[heads:])
    staged_ref[QUARTERS] = rest.astype(BF16).reshape(sources, HEAD, width)
    sent.append(send_out(staged_ref, out_ref, out_sems, QUARTERS))
    for copy in sent:
        copy.wait()


def hold_kernel(nanos_ref, _, out_ref):
    @pl.when(nanos_ref[0] > 0)
    def _():
        pl.delay(nanos_ref[0])


def mix_kernel(back_ref, tok_ref, ids_ref, weight_ref, gain_ref, shift_ref, out_ref, sum_ref):
    experts, _, width = back_ref.shape
    count, model_width = tok_ref.shape
    expert = iota((count, experts), 1)
    first, last = ids_ref[:, 0:1] == expert, ids_ref[:, 1:2] == expert
    hit = jnp.where(first | last, 1.0, 0.0)
    before = flag(iota((count, count), 1) < iota((count, count), 0))
    place = hit * (dot(before, hit.astype(BF16)) + 1.0)
    weight = jnp.where(first, weight_ref[:, 0:1], 0.0) + jnp.where(last, weight_ref[:, 1:2], 0.0)
    high = weight.astype(BF16)
    low = (weight - high.astype(F32)).astype(BF16)
    slots = experts * HEAD
    spread = flag(iota((experts, slots), 1) // HEAD == iota((experts, slots), 0))
    place = dot(place.astype(BF16), spread)
    high, low = dot(high, spread), dot(low, spread)
    column = iota((count, slots), 1)
    in_block = column % HEAD

    def chosen(condition):
        return (
            jnp.where(condition, high, 0.0).astype(BF16),
            jnp.where(condition, low, 0.0).astype(BF16),
        )

    head_high, head_low = chosen(place == (in_block + 1).astype(F32))
    second = place == (HEAD + 1 + column % REST).astype(F32)
    rest = back_ref[:, QUARTERS * HEAD :, :].reshape(slots, width)
    total = jnp.zeros((count, 1), F32)
    for q in range(QUARTERS):
        cols = slice(q * width, (q + 1) * width)
        head = back_ref[:, q * HEAD : (q + 1) * HEAD, :].reshape(slots, width)
        rest_high, rest_low = chosen(second & (in_block // REST == q))
        mixture = dot(head_high, head) + dot(rest_high, rest)
        mixture += dot(head_low, head) + dot(rest_low, rest)
        residual = residual_scale * tok_ref[:, cols].astype(F32) + mixture
        sum_ref[:, cols] = residual
        total += jnp.sum(residual, axis=-1, keepdims=True)
    center = sum_ref[...] - total / model_width
    variance = jnp.mean(center * center, axis=-1, keepdims=True)
    out_ref[...] = (center * lax.rsqrt(variance + norm_eps) * gain_ref[...] + shift_ref[...]).astype(BF16)


def body(tokens, expert_ids, group_weight, expert_share, gate_w, up_w, down_w, out_gain, out_shift):
    tok_count, model_width = tokens.shape
    ep_size = lax.axis_size("ep")
    width = model_width // QUARTERS
    block = (HEAD + REST) * QUARTERS
    hidden = gate_w.shape[1] * lax.axis_size("tp")
    buffer = jax.ShapeDtypeStruct((ep_size, block, width), BF16)
    vmem = pl.BlockSpec(memory_space=pltpu.VMEM)
    hbm = pl.BlockSpec(memory_space=pl.ANY)
    staged = pltpu.VMEM((QUARTERS + 1, ep_size, HEAD, width), BF16)
    staged_sems = pltpu.SemaphoreType.DMA((QUARTERS + 1,))
    limit = pltpu.CompilerParams(vmem_limit_bytes=32 * 2**20)
    send = pl.pallas_call(
        pack_kernel,
        out_shape=buffer,
        out_specs=hbm,
        scratch_shapes=[staged, staged_sems],
        name="pack",
    )(tokens, expert_ids.T)
    own = jnp.concatenate([gate_w[0], up_w[0], down_w[0]], axis=0)
    gathered = lax.all_gather(own, "tp", axis=0, tiled=True)
    late = (lax.axis_index("tp") % 2 == LATE).astype(jnp.int32).reshape(1)
    send = pl.pallas_call(
        hold_kernel,
        out_shape=buffer,
        in_specs=[pl.BlockSpec(memory_space=pltpu.SMEM), hbm],
        out_specs=hbm,
        input_output_aliases={1: 0},
        compiler_params=pltpu.CompilerParams(has_side_effects=True),
        name="hold",
    )(late * HOLD, send)
    received = lax.all_to_all(send, "ep", split_axis=0, concat_axis=0, tiled=True)
    pieces = [gathered.reshape(-1, 3, SLICE, model_width)]
    rows = ep_size * (HEAD + REST)
    results = pl.pallas_call(
        functools.partial(ffn_kernel, 2),
        out_shape=buffer,
        in_specs=[vmem] + [hbm] * (len(pieces) + 1),
        out_specs=hbm,
        scratch_shapes=[
            pltpu.VMEM((hidden // SLICE, 3, SLICE, model_width), BF16),
            pltpu.VMEM((rows, model_width), BF16),
            pltpu.VMEM((rows, hidden), BF16),
            staged,
            pltpu.SemaphoreType.DMA((2,)),
            staged_sems,
        ],
        input_output_aliases={1: 0},
        compiler_params=pltpu.CompilerParams(vmem_limit_bytes=ROOM),
        name="ffn",
    )(received, send, *pieces)
    back = lax.all_to_all(results, "ep", split_axis=0, concat_axis=0, tiled=True)
    share_norm = expert_share / jnp.sum(expert_share, axis=1, keepdims=True)
    route_weight = group_weight[:, None] * share_norm
    return pl.pallas_call(
        mix_kernel,
        out_shape=jax.ShapeDtypeStruct((tok_count, model_width), BF16),
        in_specs=[vmem] * 6,
        out_specs=vmem,
        scratch_shapes=[pltpu.VMEM((tok_count, model_width), F32)],
        compiler_params=limit,
        name="mix",
    )(back, tokens, expert_ids, route_weight, out_gain[None], out_shift[None])


def solution(mesh):
    placed = (
        P(("ep", "tp"), None),
        P(("ep", "tp"), None),
        P(("ep", "tp")),
        P(("ep", "tp"), None),
        P("ep", "tp", None),
        P("ep", "tp", None),
        P("ep", "tp", None),
        P(),
        P(),
    )
    return jax.shard_map(
        body, mesh=mesh, in_specs=placed, out_specs=P(("ep", "tp"), None), check_vma=False
    )
```
